32 devices in a mesh: sp: 8 (over z, y), tp: 4 (over x, core).
Axes of the slice: x: 2, y: 2, z: 4, core: 2. Of those that a mesh axis runs over, the one named last changes fastest.
Arguments:
- cotangent: bfloat16 [2048, 2048], P('sp'), may hold values from -6 to 6
- stream_in: bfloat16 [2048, 2048], P('sp'), may hold values from -6 to 6
- norm_gain: float32 [2048], replicated, may hold values from 0.1 to 1.9
- out_gate: bfloat16 [2048, 1024], P('sp', 'tp'), may hold values from -6 to 6
- in_gate: bfloat16 [2048, 1024], P('sp', 'tp'), may hold values from -6 to 6
- conv_input: bfloat16 [2048, 1024], P('sp', 'tp'), may hold values from -6 to 6
- conv_taps: float32 [3, 1024], P(None, 'tp'), may hold values from -3 to 3
- out_weight: bfloat16 [2048, 1024], P(None, 'tp'), may hold values from -0.1875 to 0.1875
- expert_gate: bfloat16 [8, 2048, 1024], P('sp', None, 'tp'), may hold values from -0.125 to 0.125
- expert_up: bfloat16 [8, 2048, 1024], P('sp', None, 'tp'), may hold values from -0.125 to 0.125
- expert_down: bfloat16 [8, 1024, 2048], P('sp', 'tp'), may hold values from -0.1875 to 0.1875
- expert_choice: int32 [2048, 2], P('sp'), may hold values from 0 to 7, all different within a row; in each aligned block of 256 rows (0 to 255, 256 to 511, ...) at most 128 rows name the same one
- route_scale: float32 [2048, 2], P('sp'), may hold values from 0.05 to 0.6
Outputs:
- grad_stream: bfloat16 [2048, 2048], P('sp', 'tp')
- grad_out_gate: bfloat16 [2048, 1024], P('sp', 'tp')
- grad_in_gate: bfloat16 [2048, 1024], P('sp', 'tp')
- grad_conv_input: bfloat16 [2048, 1024], P('sp', 'tp')
- grad_out_weight: float32 [2048, 1024], P('sp', 'tp')
- grad_expert_gate: float32 [8, 2048, 1024], P('sp', None, 'tp')
- grad_expert_up: float32 [8, 2048, 1024], P('sp', None, 'tp')
- grad_expert_down: float32 [8, 1024, 2048], P('sp', 'tp')
The draws below stay inside these ranges and needn't reach their ends.
Inputs may be any that keep to these rules, and one draw needn't show every extreme that they name: `expert_choice`: each row names two different experts. Within the rows of one device no expert is named more than 128 times, a bound that some block reaches in some devices' rows.
All inputs are finite; a program needn't handle non-finite values.
Results may differ from the reference program's by a relative error of at most 0.01.
Values may be sent and summed in bfloat16 or wider, within the bound.
A program may use at most 128 MiB of HBM per device.

```python
import math
import jax
import jax.numpy as jnp
import numpy as np
from jax import lax

D = 2048
CW = 1024
FF = 1024
TAPS = 3
TOK_DEV = 256
TOKENS = 2048
EXPERTS = 8
CAP = 128
N_SP = 8
N_TP = 4


def raised(drawn, rng, source, target, shards_of, factor):
    def block_of(dim):
        return (jnp.arange(drawn.shape[dim]) // (drawn.shape[dim] // shards_of)).reshape((-1,) + (1,) * (drawn.ndim - 1 - dim))

    first = jax.random.permutation(rng, shards_of)[block_of(target)]
    other_side = (block_of(target) + shards_of // 2) % shards_of
    return jnp.where((block_of(source) == first) | (block_of(source) == other_side), factor * drawn, drawn)


def shard_levels(rng, dims, cuts, low, top_value):
    def one(axis_at, blocks):
        heights = jax.random.uniform(jax.random.fold_in(jax.random.fold_in(rng, 6), axis_at), (blocks,), jnp.float32, low / len(cuts), top_value / len(cuts))
        return jnp.repeat(jnp.exp(heights), dims[axis_at] // blocks).reshape((-1,) + (1,) * (len(dims) - axis_at - 1))

    factor_of = one(*cuts[0])
    for cut in cuts[1:]:
        factor_of = factor_of * one(*cut)
    return factor_of


def deal_out(key, own, number, rows, count, top, reach, slope):
    sequence = jax.random.permutation(key, count)
    heavy_load, common = load_shares(count, rows * top, reach, slope, True), load_shares(count, rows * top, reach, slope, False)
    places = jnp.arange(count)

    def named(lengths, offset_by):
        used = int((lengths > 0).sum())
        fixed = max(1, used // 4)
        passed = fixed + (places - fixed + offset_by * (used - fixed)) % max(1, count - fixed)
        return jnp.zeros((count,), jnp.int32).at[sequence[jnp.where(places < fixed, places, passed)]].set(jnp.asarray(lengths, jnp.int32))

    lengths = jnp.where(number % 4 == 0, named(heavy_load, number // 4), named(common, number - number // 4 - 1))
    mixed = jax.random.permutation(jax.random.fold_in(own, 3), count)
    source_of, sink = mixed[0:count // 2 * 2:2], mixed[1:count // 2 * 2:2]
    slack = jnp.minimum(lengths[source_of] - 1, reach - lengths[sink]) // 2
    slack = jnp.where((source_of == sequence[0]) | (sink == sequence[0]) | (lengths[sink] == 0), 0, jnp.maximum(slack, 0))
    passed = jax.random.randint(jax.random.fold_in(own, 4), (count // 2,), 0, 1 << 20) % (slack + 1)
    lengths = lengths.at[source_of].add(-passed).at[sink].add(passed)
    members = jnp.searchsorted(jnp.cumsum(lengths), jnp.arange(rows * top), side="right").astype(jnp.int32)
    grid = members.reshape(top, rows).T
    grid = grid[jax.random.permutation(jax.random.fold_in(own, 1), rows)]
    offset_by = jax.random.randint(jax.random.fold_in(own, 2), (rows, 1), 0, top)
    return jnp.take_along_axis(grid, (jnp.arange(top)[None, :] + offset_by) % top, axis=1)


def load_shares(number_of, total, most, slope, full):
    loads = [(1 << 20) // math.isqrt(standing ** slope) + 1 for standing in range(1, number_of + 1)]
    largest = most if full else min(most, max(-(-total // number_of), total * loads[0] // sum(loads)))
    least = 1 if total - largest >= number_of - 1 else 0
    holding, surplus = [largest] + [least] * (number_of - 1), total - largest - least * (number_of - 1)
    while surplus > 0:
        free = [i for i in range(1, number_of) if holding[i] < largest] or [i for i in range(1, number_of) if holding[i] < most]
        pool, left = sum([loads[i] for i in free]), surplus
        for i in free:
            more = min(most - holding[i], max(1, left * loads[i] // pool), surplus)
            holding[i] = holding[i] + more
            surplus = surplus - more
    return np.array(holding)


def normal_values(rng, shape, spread, reach, cuts=(), kind=jnp.bfloat16):
    array = spread * jax.random.normal(rng, shape, jnp.float32)
    if cuts:
        array = array * shard_levels(rng, shape, cuts, -0.22, 0.18)
    return jnp.clip(array, -reach, reach).astype(kind)


def gaussian_with(own_key, extent, width, most, pieces, heavy, kind=jnp.bfloat16):
    values = width * jax.random.normal(own_key, extent, jnp.float32)
    if pieces:
        values = values * shard_levels(own_key, extent, pieces, -0.22, 0.18)
    return jnp.clip(raised(values, jax.random.fold_in(own_key, 3), *heavy), -most, most).astype(kind)


def setup_inputs(seed: int = 0) -> dict:
    streams_of = jax.random.split(jax.random.key(seed), 14)
    cotangent = gaussian_with(streams_of[0], (TOKENS, D), 1.0, 6.0, ((0, 8),), (0, 1, 8, 2.0))
    stream_in = normal_values(streams_of[1], (TOKENS, D), 1.0, 6.0, ((0, 8),))
    norm_gain = jnp.clip(1.0 + 0.18 * jax.random.normal(streams_of[2], (D,), jnp.float32), 0.1, 1.9)
    out_gate = normal_values(streams_of[3], (TOKENS, CW), 1.0, 6.0, ((0, 8), (1, 4)))
    in_gate = normal_values(streams_of[4], (TOKENS, CW), 1.0, 6.0, ((0, 8), (1, 4)))
    conv_input = normal_values(streams_of[5], (TOKENS, CW), 1.0, 6.0, ((0, 8), (1, 4)))
    conv_taps = normal_values(streams_of[6], (TAPS, CW), 0.577, 3.0, ((1, 4),), jnp.float32)
    out_weight = normal_values(streams_of[7], (D, CW), CW ** -0.5, 0.1875, ((1, 4),))
    expert_gate = normal_values(streams_of[8], (EXPERTS, D, FF), D ** -0.5, 0.125, ((0, 8), (2, 4)))
    expert_up = normal_values(streams_of[9], (EXPERTS, D, FF), D ** -0.5, 0.125, ((0, 8), (2, 4)))
    expert_down = normal_values(streams_of[10], (EXPERTS, FF, D), FF ** -0.5, 0.1875, ((0, 8), (1, 4)))
    expert_choice_keys = jax.random.split(jax.random.fold_in(streams_of[11], 1), TOKENS // TOK_DEV)
    expert_choice_turns = jax.random.permutation(jax.random.fold_in(streams_of[11], 3), TOKENS // TOK_DEV)
    expert_choice = jax.vmap(lambda own, number: deal_out(jax.random.fold_in(streams_of[11], 2), own, number, TOK_DEV, EXPERTS, 2, CAP, 2))(expert_choice_keys, expert_choice_turns).reshape((TOKENS, 2))
    route_scale = jnp.clip(0.05 + 0.55 * jax.random.uniform(streams_of[12], (TOKENS, 2), jnp.float32) ** shard_levels(streams_of[12], (TOKENS, 2), ((0, 8),), -0.2, 0.2), 0.05, 0.6)
    return {"cotangent": cotangent, "stream_in": stream_in, "norm_gain": norm_gain, "out_gate": out_gate, "in_gate": in_gate, "conv_input": conv_input, "conv_taps": conv_taps, "out_weight": out_weight, "expert_gate": expert_gate, "expert_up": expert_up, "expert_down": expert_down, "expert_choice": expert_choice, "route_scale": route_scale}


norm_eps = 1e-06

def slot_table(choice_rows, expert_count, capacity):
    flat_ids = choice_rows.reshape(-1).astype(jnp.int32)
    route_count = flat_ids.shape[0]
    onehot = (flat_ids[:, None] == jnp.arange(expert_count, dtype=jnp.int32)[None, :]).astype(jnp.int32)
    earlier = jnp.cumsum(onehot, axis=0) - onehot
    position = lax.optimization_barrier(jnp.sum(earlier * onehot, axis=1)).astype(jnp.int32)
    slot_of_route = (flat_ids * capacity + position).astype(jnp.int32)
    route_of_slot = jnp.full((expert_count * capacity,), route_count, jnp.int32)
    route_of_slot = route_of_slot.at[slot_of_route].set(jnp.arange(route_count, dtype=jnp.int32))
    return (slot_of_route, route_of_slot)

def rows_product(left, right):
    return lax.dot_general(left, right, (((0,), (0,)), ((), ())), preferred_element_type=jnp.float32)

def cols_product(left, right):
    return lax.dot_general(left, right, (((1,), (1,)), ((), ())), preferred_element_type=jnp.float32)

def reference(cotangent, stream_in, norm_gain, out_gate, in_gate, conv_input, conv_taps, out_weight, expert_gate, expert_up, expert_down, expert_choice, route_scale):
    stream = stream_in.astype(jnp.float32)
    inverse_rms = lax.rsqrt(lax.optimization_barrier(jnp.mean(stream * stream, axis=-1, keepdims=True)) + norm_eps)
    unit_stream = stream * inverse_rms
    normed = (unit_stream * norm_gain.astype(jnp.float32)).astype(jnp.bfloat16)
    capacity = 4 * TOK_DEV // N_SP
    route_count = 2 * TOK_DEV
    block_ids = expert_choice.reshape(N_SP, TOK_DEV, 2)
    tables = jax.vmap(lambda choice_block: slot_table(choice_block, EXPERTS, capacity)[1])(block_ids)
    flat_scale = route_scale.reshape(-1)
    source_base = (jnp.arange(N_SP, dtype=jnp.int32) * route_count)[:, None]
    width_tp = FF // N_TP

    def expert_step(accum, inputs):
        w_gate, w_up, w_down, expert = inputs
        chosen = lax.dynamic_slice_in_dim(tables, (expert * capacity).astype(jnp.int32), capacity, 1)
        present = chosen < route_count
        routes = (source_base + jnp.where(present, chosen, 0)).reshape(-1).astype(jnp.int32)
        present = present.reshape(-1)
        token = (routes // 2).astype(jnp.int32)
        weight = jnp.where(present, flat_scale[routes], jnp.zeros((), jnp.float32))
        scaled_cot = (cotangent[token].astype(jnp.float32) * weight[:, None]).astype(jnp.bfloat16)
        expert_rows = jnp.where(present[:, None], normed[token], jnp.zeros((), jnp.bfloat16))
        gate_pre = jnp.dot(expert_rows, w_gate, preferred_element_type=jnp.float32)
        up_pre = jnp.dot(expert_rows, w_up, preferred_element_type=jnp.float32)
        sigmoid_gate = jax.nn.sigmoid(gate_pre)
        silu_gate = gate_pre * sigmoid_gate
        hidden = (silu_gate * up_pre).astype(jnp.bfloat16)
        grad_down = rows_product(hidden, scaled_cot)
        hidden_grad = cols_product(scaled_cot, w_down)
        gate_grad = (hidden_grad * up_pre * sigmoid_gate * (1.0 + gate_pre * (1.0 - sigmoid_gate))).astype(jnp.bfloat16)
        up_grad = (hidden_grad * silu_gate).astype(jnp.bfloat16)
        grad_gate = rows_product(expert_rows, gate_grad)
        grad_up = rows_product(expert_rows, up_grad)
        slot_rows = expert_rows.shape[0]
        shares = jnp.einsum('rpf,dpf->prd', gate_grad.astype(jnp.float32).reshape(slot_rows, N_TP, width_tp), w_gate.astype(jnp.float32).reshape(D, N_TP, width_tp))
        shares = shares + jnp.einsum('rpf,dpf->prd', up_grad.astype(jnp.float32).reshape(slot_rows, N_TP, width_tp), w_up.astype(jnp.float32).reshape(D, N_TP, width_tp))
        rounded = lax.optimization_barrier(shares.astype(jnp.bfloat16))
        slot_grad = lax.optimization_barrier(jnp.sum(rounded.astype(jnp.float32), axis=0)).astype(jnp.bfloat16)
        slot_grad = lax.optimization_barrier(slot_grad)
        accum = accum.at[token].add(jnp.where(present[:, None], slot_grad.astype(jnp.float32), jnp.zeros((), jnp.float32)))
        return (accum, (grad_gate, grad_up, grad_down))
    start_accum = jnp.zeros((TOKENS, D), jnp.float32)
    accum, grads = lax.scan(expert_step, start_accum, (expert_gate, expert_up, expert_down, jnp.arange(EXPERTS, dtype=jnp.int32)))
    grad_gate, grad_up, grad_down = grads
    token_grad = lax.optimization_barrier(accum.astype(jnp.bfloat16))
    unit_grad = token_grad.astype(jnp.float32) * norm_gain.astype(jnp.float32)
    along = lax.optimization_barrier(jnp.mean(unit_stream * unit_grad, axis=-1, keepdims=True))
    stream_grad = (cotangent.astype(jnp.float32) + inverse_rms * (unit_grad - unit_stream * along)).astype(jnp.bfloat16)
    taps = conv_taps.astype(jnp.float32)
    product = in_gate.astype(jnp.float32) * conv_input.astype(jnp.float32)
    padded = jnp.pad(product, ((2, 0), (0, 0)))
    filtered = taps[0] * product + taps[1] * padded[1:-1] + taps[2] * padded[:-2]
    mixed_in = (out_gate.astype(jnp.float32) * filtered).astype(jnp.bfloat16)
    mixed_grad = jnp.dot(stream_grad, out_weight, preferred_element_type=jnp.float32)
    grad_out_gate = (mixed_grad * filtered).astype(jnp.bfloat16)
    filtered_grad = mixed_grad * out_gate.astype(jnp.float32)
    padded_grad = jnp.pad(filtered_grad, ((0, 2), (0, 0)))
    product_grad = taps[0] * filtered_grad + taps[1] * padded_grad[1:-1] + taps[2] * padded_grad[2:]
    grad_in_gate = (product_grad * conv_input.astype(jnp.float32)).astype(jnp.bfloat16)
    grad_conv_input = (product_grad * in_gate.astype(jnp.float32)).astype(jnp.bfloat16)
    grad_out_weight = rows_product(stream_grad, mixed_in)
    return (stream_grad, grad_out_gate, grad_in_gate, grad_conv_input, grad_out_weight, grad_gate, grad_up, grad_down)
```

```python
import functools

import jax
import jax.numpy as jnp
from jax import lax
from jax.experimental import pallas as pl
from jax.experimental.pallas import tpu as pltpu
from jax.sharding import PartitionSpec as P

norm_eps = 1e-06


def passed_along(value, axis, steps):
    count = lax.axis_size(axis)
    first, last = (max(0, -steps), min(count, count - steps))
    return lax.ppermute(value, axis, [(source, source + steps) for source in range(first, last)])


def slot_masks(choice_rows, expert_count, capacity):
    rows = choice_rows.shape[0]
    onehot = choice_rows[:, :, None] == jnp.arange(expert_count, dtype=jnp.int32)
    member = jnp.any(onehot, axis=1).astype(jnp.bfloat16)
    at = jnp.arange(rows, dtype=jnp.int32)
    before = (at[:, None] > at[None, :]).astype(jnp.bfloat16)
    earlier = jnp.dot(before, member, preferred_element_type=jnp.float32).astype(jnp.int32)
    position = jnp.sum(jnp.where(onehot, earlier[:, None, :], 0), axis=-1)
    slot = choice_rows * capacity + position
    slots = jnp.arange(expert_count * capacity, dtype=jnp.int32)[:, None]
    return (slots == slot[:, 0][None, :], slots == slot[:, 1][None, :])


def rows_product(left, right):
    return lax.dot_general(
        left, right, (((0,), (0,)), ((), ())), preferred_element_type=jnp.float32
    )


def cols_product(left, right):
    return lax.dot_general(
        left, right, (((1,), (1,)), ((), ())), preferred_element_type=jnp.float32
    )


MESH = pl.DeviceIdType.MESH


def remote(source, target, send_sem, recv_sem, device):
    return pltpu.make_async_remote_copy(
        src_ref=source,
        dst_ref=target,
        send_sem=send_sem,
        recv_sem=recv_sem,
        device_id=device,
        device_id_type=MESH,
    )


def columns(index, width):
    return pl.ds(pl.multiple_of(index * width, width), width)


def tp_places():
    tp, count = lax.axis_index("tp"), lax.axis_size("tp")
    cross = lax.rem(tp + count // 2, count)
    partner = tp + 1 - 2 * lax.rem(tp, 2)
    return (tp, cross, partner, lax.rem(partner + count // 2, count))


def greet(exchange, cross, partner):
    barrier = pltpu.get_barrier_semaphore()
    waits = 2
    for peer in (cross, partner):
        pl.semaphore_signal(barrier, inc=1, device_id={"tp": peer}, device_id_type=MESH)
    if exchange:
        me, n = lax.axis_index("sp"), lax.axis_size("sp")
        waits = waits + n - 1

        def greet_one(k, carry):
            peer = lax.rem(me + k, n)
            pl.semaphore_signal(barrier, inc=1, device_id={"sp": peer}, device_id_type=MESH)
            return carry

        lax.fori_loop(1, n, greet_one, 0)
    pl.semaphore_wait(barrier, waits)


def gather_kernel(n, exchange, count, *refs):
    ins, outs = refs[:count], refs[count : 2 * count]
    local, send, recv_a, recv_b, recv_near = refs[2 * count :]
    rows, width = ins[0].shape
    depth = rows // n
    tp, cross, partner, _ = tp_places()
    me = lax.axis_index("sp")
    greet(exchange, cross, partner)

    def block_of(a, block, column):
        return outs[a].at[pl.ds(pl.multiple_of(block * depth, depth), depth), columns(column, width)]

    def source(k):
        return lax.rem(me - k + n, n) if exchange else k

    def sent(a, k):
        peer = lax.rem(me + k, n)
        return remote(
            ins[a].at[pl.ds(pl.multiple_of(peer * depth, depth), depth), :],
            block_of(a, me, tp),
            send.at[0, a],
            recv_a.at[a, k],
            {"sp": peer},
        )

    def send_all(k, carry):
        for a in range(count):
            sent(a, k).start()
        return carry

    def across(a, k):
        block = block_of(a, source(k), tp)
        return remote(block, block, send.at[1, a], recv_b.at[a, k], {"tp": cross})

    def relay(k):
        for a in range(count):
            if exchange and not isinstance(k, int):
                sent(a, k).wait_recv()
            block = block_of(a, source(k), tp)
            across(a, k).start()
            remote(block, block, send.at[2, a], recv_near.at[0, a], {"tp": partner}).start()

    def forward(k):
        for a in range(count):
            across(a, k).wait_recv()
            block = block_of(a, source(k), cross)
            remote(block, block, send.at[3, a], recv_near.at[1, a], {"tp": partner}).start()

    if exchange:
        lax.fori_loop(1, n, send_all, 0)
    for a in range(count):
        if exchange:
            own = pltpu.make_async_copy(
                ins[a].at[pl.ds(pl.multiple_of(me * depth, depth), depth), :],
                block_of(a, me, tp),
                local.at[a],
            )
        else:
            own = pltpu.make_async_copy(ins[a], outs[a].at[:, columns(tp, width)], local.at[a])
        own.start()
        own.wait()
    relay(0)

    def step(k, carry):
        relay(k)
        forward(k - 1)
        return carry

    lax.fori_loop(1, n, step, 0)
    forward(n - 1)
    for a in range(count):
        whole = outs[a].at[:, columns(tp, width)]
        for kind in (0, 1):
            remote(whole, whole, send.at[2, a], recv_near.at[kind, a], {"tp": partner}).wait_recv()
        for kind in (1, 2, 3):
            remote(whole, whole, send.at[kind, a], recv_near.at[0, a], {"tp": partner}).wait_send()
        if exchange:
            rest = ins[a].at[pl.ds(0, (n - 1) * depth), :]
            remote(rest, rest, send.at[0, a], recv_near.at[0, a], {"tp": partner}).wait_send()


def gathered(parts, n, exchange, collective_id):
    count = len(parts)
    rows, width = parts[0].shape
    wide = jax.ShapeDtypeStruct((rows, width * lax.axis_size("tp")), parts[0].dtype)
    return pl.pallas_call(
        functools.partial(gather_kernel, n, exchange, count),
        out_shape=[wide] * count,
        in_specs=[pl.BlockSpec(memory_space=pl.ANY)] * count,
        out_specs=[pl.BlockSpec(memory_space=pl.ANY)] * count,
        scratch_shapes=[
            pltpu.SemaphoreType.DMA((count,)),
            pltpu.SemaphoreType.DMA((4, count)),
            pltpu.SemaphoreType.DMA((count, n)),
            pltpu.SemaphoreType.DMA((count, n)),
            pltpu.SemaphoreType.DMA((2, count)),
        ],
        compiler_params=pltpu.CompilerParams(collective_id=collective_id, has_side_effects=True),
    )(*parts)


def return_kernel(
    n,
    partial,
    out,
    near,
    far_out,
    far_in,
    total,
    local,
    send_near,
    recv_near,
    send_far,
    recv_far,
    send_out,
    recv_out,
):
    width = out.shape[2]
    tp, cross, partner, diagonal = tp_places()
    me = lax.axis_index("sp")
    greet(True, cross, partner)

    def target(k):
        return lax.rem(me + k + 1, n)

    def part(k, column):
        return partial[target(k), :, columns(column, width)].astype(jnp.float32)

    def handed(j, k):
        return remote(
            partial.at[target(k), :, columns((partner, diagonal)[j], width)],
            near.at[j, k],
            send_near.at[j],
            recv_near.at[j, k],
            {"tp": partner},
        )

    def across(k):
        return remote(far_out.at[k], far_in.at[k], send_far, recv_far.at[k], {"tp": cross})

    def hand(k, carry):
        handed(1, k).start()
        handed(0, k).start()
        return carry

    def pair(k, carry):
        handed(1, k).wait_recv()
        far_out[k] = (part(k, cross) + near[1, k].astype(jnp.float32)).astype(far_out.dtype)
        across(k).start()
        return carry

    def finish(k):
        handed(0, k).wait_recv()
        across(k).wait_recv()
        total[k] = (
            part(k, tp) + near[0, k].astype(jnp.float32) + far_in[k].astype(jnp.float32)
        ).astype(total.dtype)

    def finish_remote(k, carry):
        finish(k)
        remote(total.at[k], out.at[me], send_out, recv_out, {"sp": target(k)}).start()
        return carry

    lax.fori_loop(0, n, hand, 0)
    lax.fori_loop(0, n, pair, 0)
    lax.fori_loop(0, n - 1, finish_remote, 0)
    finish(n - 1)
    own = pltpu.make_async_copy(total.at[n - 1], out.at[me], local)
    own.start()
    own.wait()
    rest, rest_out = total.at[pl.ds(0, n - 1)], out.at[pl.ds(0, n - 1)]
    remote(rest, rest_out, send_out, recv_out, {"tp": partner}).wait()
    remote(far_out, far_in, send_far, recv_out, {"tp": cross}).wait_send()
    for j in (0, 1):
        remote(far_out, near.at[j], send_near.at[j], recv_out, {"tp": partner}).wait_send()


def returned_slots(partial, n, collective_id):
    rows, wide = partial.shape
    width, depth = wide // lax.axis_size("tp"), rows // n
    kind = partial.dtype
    return pl.pallas_call(
        functools.partial(return_kernel, n),
        out_shape=jax.ShapeDtypeStruct((n, depth, width), kind),
        in_specs=[pl.BlockSpec(memory_space=pltpu.VMEM)],
        out_specs=pl.BlockSpec(memory_space=pl.ANY),
        scratch_shapes=[
            pltpu.VMEM((2, n, depth, width), kind),
            pltpu.VMEM((n, depth, width), kind),
            pltpu.VMEM((n, depth, width), kind),
            pltpu.VMEM((n, depth, width), kind),
            pltpu.SemaphoreType.DMA,
            pltpu.SemaphoreType.DMA((2,)),
            pltpu.SemaphoreType.DMA((2, n)),
            pltpu.SemaphoreType.DMA,
            pltpu.SemaphoreType.DMA((n,)),
            pltpu.SemaphoreType.DMA,
            pltpu.SemaphoreType.DMA,
        ],
        compiler_params=pltpu.CompilerParams(
            collective_id=collective_id, has_side_effects=True, vmem_limit_bytes=32 * 1024 * 1024
        ),
    )(partial.reshape(n, depth, wide)).reshape(rows, width)


def shards(
    cotangent,
    stream_in,
    norm_gain,
    out_gate,
    in_gate,
    conv_input,
    conv_taps,
    out_weight,
    expert_gate,
    expert_up,
    expert_down,
    expert_choice,
    route_scale,
):
    sp_size = lax.axis_size("sp")
    tp_size = lax.axis_size("tp")
    rows_here = stream_in.shape[0]
    model_width = stream_in.shape[1]
    column_width = model_width // tp_size
    column_start = lax.axis_index("tp") * column_width
    capacity = 4 * rows_here // sp_size
    stream = stream_in.astype(jnp.float32)
    inverse_rms = lax.rsqrt(jnp.mean(stream * stream, axis=-1, keepdims=True) + norm_eps)
    unit_stream = stream * inverse_rms
    normed = (unit_stream * norm_gain).astype(jnp.bfloat16)
    first, second = slot_masks(expert_choice, sp_size, capacity)
    placing = (first | second).astype(jnp.bfloat16)
    weight = jnp.sum(
        jnp.where(first, route_scale[:, 0][None, :], 0.0)
        + jnp.where(second, route_scale[:, 1][None, :], 0.0),
        axis=1,
    )
    cot_cols = lax.dynamic_slice_in_dim(cotangent, column_start, column_width, 1)
    normed_cols = lax.dynamic_slice_in_dim(normed, column_start, column_width, 1)
    scaled_part = (
        jnp.dot(placing, cot_cols, preferred_element_type=jnp.float32) * weight[:, None]
    ).astype(jnp.bfloat16)
    rows_part = jnp.dot(placing, normed_cols, preferred_element_type=jnp.float32).astype(
        jnp.bfloat16
    )
    expert_rows, scaled_cot = gathered((rows_part, scaled_part), sp_size, True, 1)
    w_gate = expert_gate[0]
    w_up = expert_up[0]
    w_down = expert_down[0]
    gate_pre = jnp.dot(expert_rows, w_gate, preferred_element_type=jnp.float32)
    up_pre = jnp.dot(expert_rows, w_up, preferred_element_type=jnp.float32)
    sigmoid_gate = jax.nn.sigmoid(gate_pre)
    silu_gate = gate_pre * sigmoid_gate
    hidden = (silu_gate * up_pre).astype(jnp.bfloat16)
    hidden_grad = cols_product(scaled_cot, w_down)
    gate_grad = (
        hidden_grad * up_pre * sigmoid_gate * (1.0 + gate_pre * (1.0 - sigmoid_gate))
    ).astype(jnp.bfloat16)
    up_grad = (hidden_grad * silu_gate).astype(jnp.bfloat16)
    partial_grad = cols_product(gate_grad, w_gate) + cols_product(up_grad, w_up)
    returned = returned_slots(partial_grad.astype(jnp.bfloat16), sp_size, 2)
    grad_down = rows_product(hidden, scaled_cot)[None]
    grad_gate = rows_product(expert_rows, gate_grad)[None]
    grad_up = rows_product(expert_rows, up_grad)[None]
    product = in_gate.astype(jnp.float32) * conv_input.astype(jnp.float32)
    earlier = passed_along(product[-2:], "sp", 1)
    extended = jnp.concatenate([earlier, product], axis=0)
    filtered = conv_taps[0] * product + conv_taps[1] * extended[1:-1] + conv_taps[2] * extended[:-2]
    mixed_in = (out_gate.astype(jnp.float32) * filtered).astype(jnp.bfloat16)
    token_cols = rows_product(placing, returned).astype(jnp.bfloat16)
    pieces = max(1, rows_here // 64)
    (token_grad,) = gathered((token_cols,), pieces, False, 3)
    unit_grad = token_grad.astype(jnp.float32) * norm_gain
    along = jnp.mean(unit_stream * unit_grad, axis=-1, keepdims=True)
    stream_grad = (
        cotangent.astype(jnp.float32) + inverse_rms * (unit_grad - unit_stream * along)
    ).astype(jnp.bfloat16)
    grad_stream = lax.dynamic_slice_in_dim(stream_grad, column_start, column_width, 1)
    mixed_grad = jnp.dot(stream_grad, out_weight, preferred_element_type=jnp.float32)
    grad_out_gate = (mixed_grad * filtered).astype(jnp.bfloat16)
    filtered_grad = mixed_grad * out_gate.astype(jnp.float32)
    later = passed_along(filtered_grad[:2], "sp", -1)
    extended_grad = jnp.concatenate([filtered_grad, later], axis=0)
    product_grad = (
        conv_taps[0] * filtered_grad
        + conv_taps[1] * extended_grad[1:-1]
        + conv_taps[2] * extended_grad[2:]
    )
    grad_in_gate = (product_grad * conv_input.astype(jnp.float32)).astype(jnp.bfloat16)
    grad_conv_input = (product_grad * in_gate.astype(jnp.float32)).astype(jnp.bfloat16)
    shares = rows_product(stream_grad, mixed_in).astype(jnp.bfloat16)
    shares = shares.reshape(sp_size, model_width // sp_size, -1)
    shares = lax.all_to_all(shares, "sp", split_axis=0, concat_axis=0)
    grad_out_weight = jnp.sum(shares.astype(jnp.float32), axis=0)
    return (
        grad_stream,
        grad_out_gate,
        grad_in_gate,
        grad_conv_input,
        grad_out_weight,
        grad_gate,
        grad_up,
        grad_down,
    )


def solution(mesh):
    placed = (
        P("sp", None),
        P("sp", None),
        P(),
        P("sp", "tp"),
        P("sp", "tp"),
        P("sp", "tp"),
        P(None, "tp"),
        P(None, "tp"),
        P("sp", None, "tp"),
        P("sp", None, "tp"),
        P("sp", "tp", None),
        P("sp", None),
        P("sp", None),
    )
    return jax.shard_map(
        shards,
        mesh=mesh,
        in_specs=placed,
        out_specs=(
            P("sp", "tp"),
            P("sp", "tp"),
            P("sp", "tp"),
            P("sp", "tp"),
            P("sp", "tp"),
            P("sp", None, "tp"),
            P("sp", None, "tp"),
            P("sp", "tp", None),
        ),
        check_vma=False,
    )
```

```python
import functools

import jax
import jax.numpy as jnp
from jax import lax
from jax.experimental import pallas as pl
from jax.experimental.pallas import tpu as pltpu
from jax.sharding import PartitionSpec as P

norm_eps = 1e-06


def passed_along(value, axis, steps):
    count = lax.axis_size(axis)
    first, last = (max(0, -steps), min(count, count - steps))
    return lax.ppermute(value, axis, [(source, source + steps) for source in range(first, last)])


def slot_masks(choice_rows, expert_count, capacity):
    rows = choice_rows.shape[0]
    onehot = choice_rows[:, :, None] == jnp.arange(expert_count, dtype=jnp.int32)
    member = jnp.any(onehot, axis=1).astype(jnp.bfloat16)
    at = jnp.arange(rows, dtype=jnp.int32)
    before = (at[:, None] > at[None, :]).astype(jnp.bfloat16)
    earlier = jnp.dot(before, member, preferred_element_type=jnp.float32).astype(jnp.int32)
    position = jnp.sum(jnp.where(onehot, earlier[:, None, :], 0), axis=-1)
    slot = choice_rows * capacity + position
    slots = jnp.arange(expert_count * capacity, dtype=jnp.int32)[:, None]
    return (slots == slot[:, 0][None, :], slots == slot[:, 1][None, :])


def rows_product(left, right):
    return lax.dot_general(
        left, right, (((0,), (0,)), ((), ())), preferred_element_type=jnp.float32
    )


def cols_product(left, right):
    return lax.dot_general(
        left, right, (((1,), (1,)), ((), ())), preferred_element_type=jnp.float32
    )


MESH = pl.DeviceIdType.MESH


def remote(source, target, send_sem, recv_sem, device):
    return pltpu.make_async_remote_copy(
        src_ref=source,
        dst_ref=target,
        send_sem=send_sem,
        recv_sem=recv_sem,
        device_id=device,
        device_id_type=MESH,
    )


def columns(index, width):
    return pl.ds(pl.multiple_of(index * width, width), width)


def mirrored(me, mask, n):
    found, unit = 0, 1
    while unit < n:
        found = found + lax.rem(lax.div(me, unit) + lax.div(mask, unit), 2) * unit
        unit = 2 * unit
    return found


def tp_places():
    tp, count = lax.axis_index("tp"), lax.axis_size("tp")
    cross = lax.rem(tp + count // 2, count)
    partner = tp + 1 - 2 * lax.rem(tp, 2)
    return (tp, cross, partner, lax.rem(partner + count // 2, count))


def greet(exchange, cross, partner):
    barrier = pltpu.get_barrier_semaphore()
    waits = 2
    for peer in (cross, partner):
        pl.semaphore_signal(barrier, inc=1, device_id={"tp": peer}, device_id_type=MESH)
    if exchange:
        me, n = lax.axis_index("sp"), lax.axis_size("sp")
        waits = waits + n - 1

        def greet_one(k, carry):
            peer = lax.rem(me + k, n)
            pl.semaphore_signal(barrier, inc=1, device_id={"sp": peer}, device_id_type=MESH)
            return carry

        lax.fori_loop(1, n, greet_one, 0)
    pl.semaphore_wait(barrier, waits)


def gather_kernel(n, exchange, count, *refs):
    ins, outs = refs[:count], refs[count : 2 * count]
    local, send, recv_a, recv_b, recv_near = refs[2 * count :]
    rows, width = ins[0].shape
    depth = rows // n
    tp, cross, partner, _ = tp_places()
    me = lax.axis_index("sp")
    greet(exchange, cross, partner)

    def block_of(a, block, column):
        return outs[a].at[pl.ds(pl.multiple_of(block * depth, depth), depth), columns(column, width)]

    def source(k):
        if not exchange:
            return k
        odd = k % 2
        mask = odd * ((k + 1) // 2) + (1 - odd) * ((n - k // 2) % n)
        return mirrored(me, jnp.int32(mask), n)

    def sent(a, k):
        peer = source(k)
        return remote(
            ins[a].at[pl.ds(pl.multiple_of(peer * depth, depth), depth), :],
            block_of(a, me, tp),
            send.at[0, a],
            recv_a.at[a, k],
            {"sp": peer},
        )

    def send_all(k, carry):
        for a in range(count):
            sent(a, k).start()
        return carry

    def across(a, k):
        block = block_of(a, source(k), tp)
        return remote(block, block, send.at[1, a], recv_b.at[a, k], {"tp": cross})

    def relay(k):
        for a in range(count):
            if exchange and not isinstance(k, int):
                sent(a, k).wait_recv()
            block = block_of(a, source(k), tp)
            across(a, k).start()
            remote(block, block, send.at[2, a], recv_near.at[0, a], {"tp": partner}).start()

    def forward(k):
        for a in range(count):
            across(a, k).wait_recv()
            block = block_of(a, source(k), cross)
            remote(block, block, send.at[3, a], recv_near.at[1, a], {"tp": partner}).start()

    if exchange:
        lax.fori_loop(1, n, send_all, 0)
    for a in range(count):
        if exchange:
            own = pltpu.make_async_copy(
                ins[a].at[pl.ds(pl.multiple_of(me * depth, depth), depth), :],
                block_of(a, me, tp),
                local.at[a],
            )
        else:
            own = pltpu.make_async_copy(ins[a], outs[a].at[:, columns(tp, width)], local.at[a])
        own.start()
        own.wait()
    relay(0)

    def step(k, carry):
        relay(k)
        forward(k - 1)
        return carry

    lax.fori_loop(1, n, step, 0)
    forward(n - 1)
    for a in range(count):
        whole = outs[a].at[:, columns(tp, width)]
        for kind in (0, 1):
            remote(whole, whole, send.at[2, a], recv_near.at[kind, a], {"tp": partner}).wait_recv()
        for kind in (1, 2, 3):
            remote(whole, whole, send.at[kind, a], recv_near.at[0, a], {"tp": partner}).wait_send()
        if exchange:
            rest = ins[a].at[pl.ds(0, (n - 1) * depth), :]
            remote(rest, rest, send.at[0, a], recv_near.at[0, a], {"tp": partner}).wait_send()


def gathered(parts, n, exchange, collective_id):
    count = len(parts)
    rows, width = parts[0].shape
    wide = jax.ShapeDtypeStruct((rows, width * lax.axis_size("tp")), parts[0].dtype)
    return pl.pallas_call(
        functools.partial(gather_kernel, n, exchange, count),
        out_shape=[wide] * count,
        in_specs=[pl.BlockSpec(memory_space=pl.ANY)] * count,
        out_specs=[pl.BlockSpec(memory_space=pl.ANY)] * count,
        scratch_shapes=[
            pltpu.SemaphoreType.DMA((count,)),
            pltpu.SemaphoreType.DMA((4, count)),
            pltpu.SemaphoreType.DMA((count, n)),
            pltpu.SemaphoreType.DMA((count, n)),
            pltpu.SemaphoreType.DMA((2, count)),
        ],
        compiler_params=pltpu.CompilerParams(collective_id=collective_id, has_side_effects=True),
    )(*parts)


def return_kernel(
    n,
    partial,
    out,
    near,
    far_out,
    far_in,
    total,
    local,
    send_near,
    recv_near,
    send_far,
    recv_far,
    send_out,
    recv_out,
):
    width = out.shape[2]
    tp, cross, partner, diagonal = tp_places()
    me = lax.axis_index("sp")
    greet(True, cross, partner)

    def target(k):
        return mirrored(me, jnp.int32(n - 1 - k), n)

    def part(k, column):
        return partial[target(k), :, columns(column, width)].astype(jnp.float32)

    def handed(j, k):
        return remote(
            partial.at[target(k), :, columns((partner, diagonal)[j], width)],
            near.at[j, k],
            send_near.at[j],
            recv_near.at[j, k],
            {"tp": partner},
        )

    def across(k):
        return remote(far_out.at[k], far_in.at[k], send_far, recv_far.at[k], {"tp": cross})

    def hand(k, carry):
        handed(1, k).start()
        handed(0, k).start()
        return carry

    def pair(k, carry):
        handed(1, k).wait_recv()
        far_out[k] = (part(k, cross) + near[1, k].astype(jnp.float32)).astype(far_out.dtype)
        across(k).start()
        return carry

    def finish(k):
        handed(0, k).wait_recv()
        across(k).wait_recv()
        total[k] = (
            part(k, tp) + near[0, k].astype(jnp.float32) + far_in[k].astype(jnp.float32)
        ).astype(total.dtype)

    def finish_remote(k, carry):
        finish(k)
        remote(total.at[k], out.at[me], send_out, recv_out, {"sp": target(k)}).start()
        return carry

    lax.fori_loop(0, n, hand, 0)
    lax.fori_loop(0, n, pair, 0)
    lax.fori_loop(0, n - 1, finish_remote, 0)
    finish(n - 1)
    own = pltpu.make_async_copy(total.at[n - 1], out.at[me], local)
    own.start()
    own.wait()
    rest, rest_out = total.at[pl.ds(0, n - 1)], out.at[pl.ds(0, n - 1)]
    remote(rest, rest_out, send_out, recv_out, {"tp": partner}).wait()
    remote(far_out, far_in, send_far, recv_out, {"tp": cross}).wait_send()
    for j in (0, 1):
        remote(far_out, near.at[j], send_near.at[j], recv_out, {"tp": partner}).wait_send()


def returned_slots(partial, n, collective_id):
    rows, wide = partial.shape
    width, depth = wide // lax.axis_size("tp"), rows // n
    kind = partial.dtype
    return pl.pallas_call(
        functools.partial(return_kernel, n),
        out_shape=jax.ShapeDtypeStruct((n, depth, width), kind),
        in_specs=[pl.BlockSpec(memory_space=pltpu.VMEM)],
        out_specs=pl.BlockSpec(memory_space=pl.ANY),
        scratch_shapes=[
            pltpu.VMEM((2, n, depth, width), kind),
            pltpu.VMEM((n, depth, width), kind),
            pltpu.VMEM((n, depth, width), kind),
            pltpu.VMEM((n, depth, width), kind),
            pltpu.SemaphoreType.DMA,
            pltpu.SemaphoreType.DMA((2,)),
            pltpu.SemaphoreType.DMA((2, n)),
            pltpu.SemaphoreType.DMA,
            pltpu.SemaphoreType.DMA((n,)),
            pltpu.SemaphoreType.DMA,
            pltpu.SemaphoreType.DMA,
        ],
        compiler_params=pltpu.CompilerParams(
            collective_id=collective_id, has_side_effects=True, vmem_limit_bytes=32 * 1024 * 1024
        ),
    )(partial.reshape(n, depth, wide)).reshape(rows, width)


def shards(
    cotangent,
    stream_in,
    norm_gain,
    out_gate,
    in_gate,
    conv_input,
    conv_taps,
    out_weight,
    expert_gate,
    expert_up,
    expert_down,
    expert_choice,
    route_scale,
):
    sp_size = lax.axis_size("sp")
    tp_size = lax.axis_size("tp")
    rows_here = stream_in.shape[0]
    model_width = stream_in.shape[1]
    column_width = model_width // tp_size
    column_start = lax.axis_index("tp") * column_width
    capacity = 4 * rows_here // sp_size
    stream = stream_in.astype(jnp.float32)
    inverse_rms = lax.rsqrt(jnp.mean(stream * stream, axis=-1, keepdims=True) + norm_eps)
    unit_stream = stream * inverse_rms
    normed = (unit_stream * norm_gain).astype(jnp.bfloat16)
    first, second = slot_masks(expert_choice, sp_size, capacity)
    placing = (first | second).astype(jnp.bfloat16)
    weight = jnp.sum(
        jnp.where(first, route_scale[:, 0][None, :], 0.0)
        + jnp.where(second, route_scale[:, 1][None, :], 0.0),
        axis=1,
    )
    cot_cols = lax.dynamic_slice_in_dim(cotangent, column_start, column_width, 1)
    normed_cols = lax.dynamic_slice_in_dim(normed, column_start, column_width, 1)
    scaled_part = (
        jnp.dot(placing, cot_cols, preferred_element_type=jnp.float32) * weight[:, None]
    ).astype(jnp.bfloat16)
    rows_part = jnp.dot(placing, normed_cols, preferred_element_type=jnp.float32).astype(
        jnp.bfloat16
    )
    expert_rows, scaled_cot = gathered((rows_part, scaled_part), sp_size, True, 1)
    w_gate = expert_gate[0]
    w_up = expert_up[0]
    w_down = expert_down[0]
    gate_pre = jnp.dot(expert_rows, w_gate, preferred_element_type=jnp.float32)
    up_pre = jnp.dot(expert_rows, w_up, preferred_element_type=jnp.float32)
    sigmoid_gate = jax.nn.sigmoid(gate_pre)
    silu_gate = gate_pre * sigmoid_gate
    hidden = (silu_gate * up_pre).astype(jnp.bfloat16)
    hidden_grad = cols_product(scaled_cot, w_down)
    gate_grad = (
        hidden_grad * up_pre * sigmoid_gate * (1.0 + gate_pre * (1.0 - sigmoid_gate))
    ).astype(jnp.bfloat16)
    up_grad = (hidden_grad * silu_gate).astype(jnp.bfloat16)
    partial_grad = cols_product(gate_grad, w_gate) + cols_product(up_grad, w_up)
    returned = returned_slots(partial_grad.astype(jnp.bfloat16), sp_size, 2)
    grad_down = rows_product(hidden, scaled_cot)[None]
    grad_gate = rows_product(expert_rows, gate_grad)[None]
    grad_up = rows_product(expert_rows, up_grad)[None]
    product = in_gate.astype(jnp.float32) * conv_input.astype(jnp.float32)
    earlier = passed_along(product[-2:], "sp", 1)
    extended = jnp.concatenate([earlier, product], axis=0)
    filtered = conv_taps[0] * product + conv_taps[1] * extended[1:-1] + conv_taps[2] * extended[:-2]
    mixed_in = (out_gate.astype(jnp.float32) * filtered).astype(jnp.bfloat16)
    token_cols = rows_product(placing, returned).astype(jnp.bfloat16)
    pieces = max(1, rows_here // 64)
    (token_grad,) = gathered((token_cols,), pieces, False, 3)
    unit_grad = token_grad.astype(jnp.float32) * norm_gain
    along = jnp.mean(unit_stream * unit_grad, axis=-1, keepdims=True)
    stream_grad = (
        cotangent.astype(jnp.float32) + inverse_rms * (unit_grad - unit_stream * along)
    ).astype(jnp.bfloat16)
    grad_stream = lax.dynamic_slice_in_dim(stream_grad, column_start, column_width, 1)
    mixed_grad = jnp.dot(stream_grad, out_weight, preferred_element_type=jnp.float32)
    grad_out_gate = (mixed_grad * filtered).astype(jnp.bfloat16)
    filtered_grad = mixed_grad * out_gate.astype(jnp.float32)
    later = passed_along(filtered_grad[:2], "sp", -1)
    extended_grad = jnp.concatenate([filtered_grad, later], axis=0)
    product_grad = (
        conv_taps[0] * filtered_grad
        + conv_taps[1] * extended_grad[1:-1]
        + conv_taps[2] * extended_grad[2:]
    )
    grad_in_gate = (product_grad * conv_input.astype(jnp.float32)).astype(jnp.bfloat16)
    grad_conv_input = (product_grad * in_gate.astype(jnp.float32)).astype(jnp.bfloat16)
    shares = rows_product(stream_grad, mixed_in).astype(jnp.bfloat16)
    shares = shares.reshape(sp_size, model_width // sp_size, -1)
    shares = lax.all_to_all(shares, "sp", split_axis=0, concat_axis=0)
    grad_out_weight = jnp.sum(shares.astype(jnp.float32), axis=0)
    return (
        grad_stream,
        grad_out_gate,
        grad_in_gate,
        grad_conv_input,
        grad_out_weight,
        grad_gate,
        grad_up,
        grad_down,
    )


def solution(mesh):
    placed = (
        P("sp", None),
        P("sp", None),
        P(),
        P("sp", "tp"),
        P("sp", "tp"),
        P("sp", "tp"),
        P(None, "tp"),
        P(None, "tp"),
        P("sp", None, "tp"),
        P("sp", None, "tp"),
        P("sp", "tp", None),
        P("sp", None),
        P("sp", None),
    )
    return jax.shard_map(
        shards,
        mesh=mesh,
        in_specs=placed,
        out_specs=(
            P("sp", "tp"),
            P("sp", "tp"),
            P("sp", "tp"),
            P("sp", "tp"),
            P("sp", "tp"),
            P("sp", None, "tp"),
            P("sp", None, "tp"),
            P("sp", "tp", None),
        ),
        check_vma=False,
    )
```
